32 devices in a mesh: kv: 8 (over z, y), tp: 4 (over x, core).
Axes of the slice: x: 2, y: 2, z: 4, core: 2. Of those that a mesh axis runs over, the one named last changes fastest.
Arguments:
- tokens: bfloat16 [128, 4096], P('kv'), may hold values from -6 to 6
- dec_tokens: bfloat16 [8, 4096], P('kv'), may hold values from -6 to 6
- norm_gain: float32 [4096], replicated, may hold values from 0.1 to 1.9
- w_query: bfloat16 [2, 4096, 1024], P(None, None, 'tp'), may hold values from -0.09375 to 0.09375
- w_key: bfloat16 [2, 4096, 1024], P(None, None, 'tp'), may hold values from -0.15625 to 0.15625
- w_value: bfloat16 [4096, 2048], P(None, 'tp'), may hold values from -0.09375 to 0.09375
- w_out: bfloat16 [2048, 4096], P('tp'), may hold values from -0.125 to 0.125
- head_gain: float32 [256], replicated, may hold values from 0.1 to 1.9
- mix_lambda: float32 [8], P('tp'), may hold values from 0.3 to 0.8
- ctx_keys: bfloat16 [2, 8192, 1024], P(None, 'kv', 'tp'), may hold values from -600 to 600
- ctx_values: bfloat16 [8192, 2048], P('kv', 'tp'), may hold values from -6 to 6
- dec_keys: bfloat16 [2, 8, 2048, 1024], P(None, 'kv', None, 'tp'), may hold values from -600 to 600
- dec_values: bfloat16 [8, 2048, 2048], P('kv', None, 'tp'), may hold values from -6 to 6
- dec_len: int32 [8], P('kv'), may hold values from 256 to 2048, as said below
Outputs:
- piece_out: bfloat16 [128, 4096], P('kv', 'tp')
- dec_out: bfloat16 [8, 4096], P('kv', 'tp')
The draws below stay inside these ranges and needn't reach their ends.
Inputs may be any that keep to these rules, and one draw needn't show every extreme that they name: `dec_len`: some decoding sequence has exactly 2048 cached positions.
All inputs are finite; a program needn't handle non-finite values.
Results may differ from the reference program's by a relative error of at most 0.03.
The reference program's roundings to bfloat16 on the way count: a program that leaves them out, or rounds other values in their place, can miss the bound.
Values may be sent and summed in bfloat16 or wider, within the bound.
No kernel may reach another device: no remote copies, remote signals or barrier semaphores. Data moves between devices by JAX's collectives and lax.ppermute only.
A program may use at most 64 MiB of HBM per device.

```python
import jax
import jax.numpy as jnp
from jax import lax

D = 4096
HEADS = 8
DH = 128
DLEN = 2048
P_SIZE = 128
CTX = 8192
DECS = 8
N_TP = 4


def key_field(key, shape):
    base = jnp.clip(jax.random.normal(key, shape, jnp.float32), -6.0, 6.0) * 1.75
    return base.astype(jnp.bfloat16)


def draw_ctx_keys(key, part):
    return key_field(key, (2, CTX, HEADS * DH))


def draw_dec_keys(key, part):
    return key_field(key, (2, DECS, DLEN, HEADS * DH))


def draw_dec_len(key, part):
    lengths = jax.random.randint(key, (DECS,), DLEN // 8, DLEN + 1)
    chosen = jax.random.randint(jax.random.fold_in(key, 3), (), 0, DECS)
    return jnp.where(jnp.arange(DECS) == chosen, DLEN, lengths).astype(jnp.int32)


def block_scale(stream_key, shape, cuts, smallest, largest):
    def one(axis_at, blocks):
        heights = jax.random.uniform(jax.random.fold_in(jax.random.fold_in(stream_key, 6), axis_at), (blocks,), jnp.float32, smallest / len(cuts), largest / len(cuts))
        return jnp.repeat(jnp.exp(heights), shape[axis_at] // blocks).reshape((-1,) + (1,) * (len(shape) - axis_at - 1))

    loudness = one(*cuts[0])
    for cut in cuts[1:]:
        loudness = loudness * one(*cut)
    return loudness


def bell_draw(key, extent, scale, bound, shards=(), kind=jnp.bfloat16):
    loudness = block_scale(key, extent, shards, -0.22, 0.18) if shards else 1.0
    values = jax.random.normal(key, extent, jnp.float32) * scale * loudness
    return jnp.minimum(jnp.maximum(values, -bound), bound).astype(kind)


def setup_inputs(seed: int = 0) -> dict:
    seeds = jax.random.split(jax.random.key(seed), 15)
    return {
        "tokens": bell_draw(seeds[0], (P_SIZE, D), 1.0, 6.0, ((0, 8),)),
        "dec_tokens": bell_draw(seeds[1], (DECS, D), 1.0, 6.0, ((0, 8),)),
        "norm_gain": jnp.clip(1.0 + 0.18 * jax.random.normal(seeds[2], (D,), jnp.float32), 0.1, 1.9),
        "w_query": bell_draw(seeds[3], (2, D, HEADS * DH), D ** -0.5, 0.09375, ((2, 4),)),
        "w_key": bell_draw(seeds[4], (2, D, HEADS * DH), (D // 3) ** -0.5, 0.15625, ((2, 4),)),
        "w_value": bell_draw(seeds[5], (D, HEADS * 2 * DH), D ** -0.5, 0.09375, ((1, 4),)),
        "w_out": bell_draw(seeds[6], (HEADS * 2 * DH, D), (HEADS * 2 * DH) ** -0.5, 0.125, ((0, 4),)),
        "head_gain": jnp.clip(1.0 + 0.18 * jax.random.normal(seeds[7], (2 * DH,), jnp.float32), 0.1, 1.9),
        "mix_lambda": jnp.clip(0.3 + 0.5 * jax.random.uniform(seeds[8], (HEADS,), jnp.float32) ** block_scale(seeds[8], (HEADS,), ((0, 4),), -0.2, 0.2), 0.3, 0.8),
        "ctx_keys": draw_ctx_keys(jax.random.fold_in(seeds[14], 71), 0),
        "ctx_values": bell_draw(seeds[10], (CTX, HEADS * 2 * DH), 1.0, 6.0, ((0, 8), (1, 4))),
        "dec_keys": draw_dec_keys(jax.random.fold_in(seeds[14], 71), 0),
        "dec_values": bell_draw(seeds[12], (DECS, DLEN, HEADS * 2 * DH), 1.0, 6.0, ((0, 8), (2, 4))),
        "dec_len": draw_dec_len(jax.random.fold_in(seeds[14], 71), 0),
    }


epsilon = 1e-06

def input_rows(rows, norm_gain, w_query, w_key, w_value):
    xf = rows.astype(jnp.float32)
    normed = (xf * lax.rsqrt(lax.optimization_barrier(jnp.mean(xf * xf, axis=-1, keepdims=True)) + epsilon) * norm_gain).astype(jnp.bfloat16)
    query = jnp.stack([jnp.dot(normed, w_query[c], preferred_element_type=jnp.float32) for c in range(2)], 1).astype(jnp.bfloat16)
    keys = jnp.stack([jnp.dot(normed, w_key[c], preferred_element_type=jnp.float32) for c in range(2)], 1).astype(jnp.bfloat16)
    value = jnp.dot(normed, w_value, preferred_element_type=jnp.float32).astype(jnp.bfloat16)
    return (query, keys, value)

def reference(tokens, dec_tokens, norm_gain, w_query, w_key, w_value, w_out, head_gain, mix_lambda, ctx_keys, ctx_values, dec_keys, dec_values, dec_len):
    scale = DH ** (-0.5)
    p_query, p_keys, p_value = input_rows(tokens, norm_gain, w_query, w_key, w_value)
    d_query, d_keys, d_value = input_rows(dec_tokens, norm_gain, w_query, w_key, w_value)
    all_keys = jnp.concatenate([ctx_keys.reshape(2, CTX, HEADS, DH), p_keys.reshape(P_SIZE, 2, HEADS, DH).transpose(1, 0, 2, 3)], axis=1)
    all_keys = all_keys.transpose(2, 0, 1, 3)
    all_values = jnp.concatenate([ctx_values.reshape(CTX, HEADS, 2 * DH), p_value.reshape(P_SIZE, HEADS, 2 * DH)], axis=0)
    all_values = all_values.transpose(1, 0, 2)
    key_pos = jnp.concatenate([jnp.full((CTX,), -1, jnp.int32), jnp.arange(P_SIZE, dtype=jnp.int32)])
    heads_query = p_query.reshape(P_SIZE, 2, HEADS, DH).transpose(2, 1, 0, 3)
    block = 1
    for size in (256, 128, 64, 32, 16, 8, 4, 2, 1):
        if P_SIZE % size == 0 and block == 1:
            block = size
    blocks = P_SIZE // block

    def one_head(args):
        query_h, keys_h, values_h, lam = args
        query_b = query_h.reshape(2, blocks, block, DH).transpose(1, 0, 2, 3)
        pos_b = jnp.arange(P_SIZE, dtype=jnp.int32).reshape(blocks, block)

        def one_block(inner):
            qb, qpos = inner
            valid = key_pos[None, :] <= qpos[:, None]
            probs = []
            for c in range(2):
                scores = jnp.dot(qb[c], keys_h[c].T, preferred_element_type=jnp.float32) * scale
                scores = jnp.where(valid, scores, -jnp.inf)
                top = lax.optimization_barrier(jnp.max(scores, axis=-1, keepdims=True))
                expo = jnp.exp(scores - top)
                probs.append(expo / lax.optimization_barrier(jnp.sum(expo, axis=-1, keepdims=True)))
            weights = (probs[0] - lam * probs[1]).astype(jnp.bfloat16)
            return jnp.dot(weights, values_h, preferred_element_type=jnp.float32)
        return lax.map(one_block, (query_b, pos_b)).reshape(P_SIZE, 2 * DH)
    piece_att = lax.map(one_head, (heads_query, all_keys, all_values, mix_lambda)).transpose(1, 0, 2)

    def one_seq(args):
        query_b, dk_b, dv_b, new_k, new_v, length = args
        keys_b = jnp.concatenate([dk_b.reshape(2, DLEN, HEADS, DH), new_k.reshape(2, 1, HEADS, DH)], axis=1)
        vals_b = jnp.concatenate([dv_b.reshape(DLEN, HEADS, 2 * DH), new_v.reshape(1, HEADS, 2 * DH)], axis=0)
        slot = jnp.arange(DLEN + 1, dtype=jnp.int32)
        valid = (slot < length) | (slot == DLEN)
        probs = []
        for c in range(2):
            scores = jnp.einsum('hd,jhd->hj', query_b[c].reshape(HEADS, DH).astype(jnp.float32), keys_b[c].astype(jnp.float32)) * scale
            scores = jnp.where(valid[None, :], scores, -jnp.inf)
            top = lax.optimization_barrier(jnp.max(scores, axis=-1, keepdims=True))
            expo = jnp.exp(scores - top)
            probs.append(expo / lax.optimization_barrier(jnp.sum(expo, axis=-1, keepdims=True)))
        weights = (probs[0] - mix_lambda[:, None] * probs[1]).astype(jnp.bfloat16)
        return jnp.einsum('hj,jhe->he', weights.astype(jnp.float32), vals_b.astype(jnp.float32))
    dec_keys_seq = dec_keys.transpose(1, 0, 2, 3)
    dec_att = lax.map(one_seq, (d_query, dec_keys_seq, dec_values, d_keys, d_value, dec_len))

    def head_norm(att):
        normed = att * lax.rsqrt(lax.optimization_barrier(jnp.mean(att * att, axis=-1, keepdims=True)) + epsilon) * head_gain
        return normed.astype(jnp.bfloat16).reshape(att.shape[0], HEADS * 2 * DH)

    def project(heads_out):
        group = HEADS // N_TP * 2 * DH
        total = jnp.zeros((heads_out.shape[0], D), jnp.float32)
        for g in range(N_TP):
            part = jnp.dot(heads_out[:, g * group:(g + 1) * group], w_out[g * group:(g + 1) * group], preferred_element_type=jnp.float32)
            part = lax.optimization_barrier(part.astype(jnp.bfloat16))
            total = total + part.astype(jnp.float32)
        return total.astype(jnp.bfloat16)
    return (project(head_norm(piece_att)), project(head_norm(dec_att)))
```

```python
import functools

import jax
import jax.numpy as jnp
from jax import lax
from jax.experimental import pallas as pl
from jax.experimental.pallas import tpu as pltpu
from jax.sharding import PartitionSpec as P

DH = 128
LANES = 128
epsilon = 1e-06
F32 = jnp.float32
BF16 = jnp.bfloat16


def up(n, m):
    return -(-n // m) * m


def dot(a, b):
    return lax.dot_general(a, b, (((1,), (0,)), ((), ())), preferred_element_type=F32)


def dot_t(a, b):
    return lax.dot_general(a, b, (((1,), (1,)), ((), ())), preferred_element_type=F32)


def vmem():
    return pl.BlockSpec(memory_space=pltpu.VMEM)


def smem():
    return pl.BlockSpec(memory_space=pltpu.SMEM)


def hbm():
    return pl.BlockSpec(memory_space=pl.ANY)


def params(mib):
    return pltpu.CompilerParams(vmem_limit_bytes=mib * 1024 * 1024)


def split3(x):
    hi = x.astype(BF16)
    rest = x - hi.astype(F32)
    mid = rest.astype(BF16)
    low = (rest - mid.astype(F32)).astype(BF16)
    return hi.astype(F32), mid.astype(F32), low.astype(F32)


def query_kernel(tok, dec, gain, wq, q_all, q_dec, normed, wbuf, sems, *, copies, steps):
    parts, depth, width = wq.shape
    step = depth // steps
    moves = []
    for c in range(parts):
        for k in range(steps):
            move = pltpu.make_async_copy(
                wq.at[c, pl.ds(k * step, step)], wbuf.at[c, pl.ds(k * step, step)], sems.at[c, k]
            )
            move.start()
            moves.append(move)
    piece_rows = tok.shape[0]
    dec_rows = dec.shape[0]

    def norm(x):
        xf = x.astype(F32)
        mean = jnp.mean(xf * xf, axis=-1, keepdims=True)
        return (xf * lax.rsqrt(mean + epsilon) * gain[...]).astype(BF16)

    normed[...] = jnp.zeros(normed.shape, BF16)
    normed[:piece_rows] = norm(tok[...])
    normed[piece_rows : piece_rows + dec_rows] = norm(dec[...])
    for c in range(parts):
        acc = jnp.zeros((normed.shape[0], width), F32)
        for k in range(steps):
            moves[c * steps + k].wait()
            cut = slice(k * step, (k + 1) * step)
            acc = acc + dot(normed[:, cut], wbuf[c, cut])
        out = acc.astype(BF16)
        cols = slice(c * width, (c + 1) * width)
        for i in range(copies):
            q_all[i, :, cols] = out[:piece_rows]
        q_dec[:, cols] = out[piece_rows:]


def attend_kernel(
    lens, lam, normed, wk, wv, q_all, q_dec, ck, cv, dk, dv, send, dec_att, own_k, own_v,
    *, piece_rows, dec_rows, axis,
):
    scale = DH ** (-0.5)
    width = wk.shape[2]
    heads = width // DH
    total = q_all.shape[0]
    for c in range(2):
        own_k[:, c * width : (c + 1) * width] = dot(normed[...], wk[c]).astype(BF16)
    own_v[...] = dot(normed[...], wv[...]).astype(BF16)

    first = lax.axis_index(axis) * piece_rows
    block = min(128, total)

    def rows(at):
        qpos = at + lax.broadcasted_iota(jnp.int32, (block, piece_rows), 0)
        kpos = first + lax.broadcasted_iota(jnp.int32, (block, piece_rows), 1)
        keep = kpos <= qpos
        lane = lax.broadcasted_iota(jnp.int32, (block, LANES), 1)
        stats = jnp.zeros((block, LANES), F32)
        for h in range(heads):
            vcols = slice(h * 2 * DH, (h + 1) * 2 * DH)
            for c in range(2):
                cols = slice(h * DH, (h + 1) * DH)
                qcols = slice(c * width + h * DH, c * width + (h + 1) * DH)
                q = q_all[pl.ds(at, block), qcols]
                far = dot_t(q, ck[c, :, cols]) * scale
                near = dot_t(q, own_k[:piece_rows, qcols]) * scale
                near = jnp.where(keep, near, -jnp.inf)
                top = jnp.maximum(
                    jnp.max(far, axis=-1, keepdims=True), jnp.max(near, axis=-1, keepdims=True)
                )
                far = jnp.exp(far - top)
                near = jnp.exp(near - top)
                tot = jnp.sum(far, axis=-1, keepdims=True) + jnp.sum(near, axis=-1, keepdims=True)
                out = dot(far.astype(BF16), cv[:, vcols])
                out = out + dot(near.astype(BF16), own_v[:piece_rows, vcols])
                j = 2 * h + c
                base = j * 2 * DH
                send[pl.ds(at, block), base : base + 2 * DH] = out.astype(BF16)
                for g, (a, b) in enumerate(zip(split3(top), split3(tot))):
                    stats = jnp.where(lane == 32 * g + j, a, stats)
                    stats = jnp.where(lane == 32 * g + 2 * heads + j, b, stats)
        base = 4 * width
        send[pl.ds(at, block), base : base + LANES] = stats.astype(BF16)

    if total == block:
        rows(0)
    else:

        def step(i, carry):
            rows(i * block)
            return carry

        lax.fori_loop(0, total // block, step, 0)

    slots = dk.shape[2]
    pad = q_dec.shape[0]
    pos = lax.broadcasted_iota(jnp.int32, (pad, slots), 1)
    row = lax.broadcasted_iota(jnp.int32, (pad, 2 * DH), 0)
    for h in range(heads):
        vcols = slice(h * 2 * DH, (h + 1) * 2 * DH)
        merged = jnp.zeros((pad, 2 * DH), F32)
        for b in range(dec_rows):
            fars, nears = [], []
            for c in range(2):
                cols = slice(h * DH, (h + 1) * DH)
                qcols = slice(c * width + h * DH, c * width + (h + 1) * DH)
                q = q_dec[:, qcols]
                far = dot_t(q, dk[c, b, :, cols]) * scale
                far = jnp.where(pos < lens[b], far, -jnp.inf)
                k = own_k[piece_rows:, qcols].astype(F32)
                near = jnp.sum(q.astype(F32) * k, axis=-1, keepdims=True) * scale
                top = jnp.maximum(jnp.max(far, axis=-1, keepdims=True), near)
                far = jnp.exp(far - top)
                near = jnp.exp(near - top)
                tot = jnp.sum(far, axis=-1, keepdims=True) + near
                fars.append(far / tot)
                nears.append(near / tot)
            far_w = (fars[0] - lam[h] * fars[1]).astype(BF16)
            near_w = (nears[0] - lam[h] * nears[1]).astype(BF16)
            out = dot(far_w, dv[b, :, vcols])
            out = out + near_w.astype(F32) * own_v[piece_rows:, vcols].astype(F32)
            merged = jnp.where(row == b, out, merged)
        dec_att[:, vcols] = merged


def project_kernel(lam, got, dec_att, gain, wo, out, heads_out, *, dec_rows, parts):
    peers, piece_rows, _ = got.shape
    heads = dec_att.shape[1] // (2 * DH)
    base = heads * 4 * DH
    stats = got[:, :, base : base + LANES].astype(F32).reshape(peers * piece_rows, LANES)
    stats = stats + (pltpu.roll(stats, LANES - 32, 1) + pltpu.roll(stats, LANES - 64, 1))
    tots = pltpu.roll(stats, LANES - 2 * heads, 1).reshape(peers, piece_rows, LANES)
    tops = stats.reshape(peers, piece_rows, LANES)
    scale = jnp.exp(tops - jnp.max(tops, axis=0, keepdims=True))
    denom = jnp.sum(scale * tots, axis=0, keepdims=True)
    coef = scale / denom

    def head_norm(att):
        mean = jnp.mean(att * att, axis=-1, keepdims=True)
        return (att * lax.rsqrt(mean + epsilon) * gain[...]).astype(BF16)

    for h in range(heads):
        vcols = slice(h * 2 * DH, (h + 1) * 2 * DH)
        sums = []
        for c in range(2):
            j = 2 * h + c
            acc = jnp.zeros((piece_rows, 2 * DH), F32)
            for s in range(peers):
                part = got[s, :, j * 2 * DH : (j + 1) * 2 * DH].astype(F32)
                acc = acc + coef[s, :, j : j + 1] * part
            sums.append(acc)
        heads_out[:piece_rows, vcols] = head_norm(sums[0] - lam[h] * sums[1])
        heads_out[piece_rows:, vcols] = head_norm(dec_att[:, vcols])
    cols = wo.shape[1] // parts
    chunks = cols // LANES
    for p in range(parts):
        part = dot(heads_out[...], wo[:, p * cols : (p + 1) * cols])
        out[p, :, :cols] = part[:piece_rows].astype(BF16)
        out[p, :, cols:] = jnp.zeros((piece_rows, out.shape[2] - cols), BF16)
        for b in range(dec_rows):
            for k in range(chunks):
                at = b * chunks + k
                lanes = cols + (at // piece_rows) * LANES
                r = at % piece_rows
                row = part[piece_rows + b : piece_rows + b + 1, k * LANES : (k + 1) * LANES]
                out[p, r : r + 1, lanes : lanes + LANES] = row.astype(BF16)


def sum_kernel(*refs, dec_rows):
    *ins, piece, dec = refs
    cols = piece.shape[1]
    piece_rows = piece.shape[0]
    chunks = cols // LANES
    total = ins[0][...].astype(F32)
    for ref in ins[1:]:
        total = total + ref[...].astype(F32)
    out = total.astype(BF16)
    piece[...] = out[:, :cols]
    for b in range(dec_rows):
        for k in range(chunks):
            at = b * chunks + k
            lanes = cols + (at // piece_rows) * LANES
            r = at % piece_rows
            dec[b : b + 1, k * LANES : (k + 1) * LANES] = out[r : r + 1, lanes : lanes + LANES]


def body(
    tokens, dec_tokens, norm_gain, w_query, w_key, w_value, w_out, head_gain, mix_lambda,
    ctx_keys, ctx_values, dec_keys, dec_values, dec_len, *, n_kv, n_tp,
):
    piece_rows, model = tokens.shape
    dec_rows = dec_tokens.shape[0]
    width = w_query.shape[2]
    pad = up(dec_rows, 16)
    rows = piece_rows + pad
    steps = 4
    q_send, q_dec, normed = pl.pallas_call(
        functools.partial(query_kernel, copies=n_kv, steps=steps),
        out_shape=(
            jax.ShapeDtypeStruct((n_kv, piece_rows, 2 * width), BF16),
            jax.ShapeDtypeStruct((pad, 2 * width), BF16),
            jax.ShapeDtypeStruct((rows, model), BF16),
        ),
        in_specs=[vmem(), vmem(), vmem(), hbm()],
        out_specs=(vmem(), vmem(), vmem()),
        scratch_shapes=[
            pltpu.VMEM(w_query.shape, BF16),
            pltpu.SemaphoreType.DMA((2, steps)),
        ],
        compiler_params=params(12),
        name="query_proj",
    )(tokens, dec_tokens, norm_gain.reshape(1, model), w_query)
    q_all = lax.all_to_all(q_send, "kv", 0, 0).reshape(n_kv * piece_rows, 2 * width)
    send, dec_att = pl.pallas_call(
        functools.partial(attend_kernel, piece_rows=piece_rows, dec_rows=dec_rows, axis="kv"),
        out_shape=(
            jax.ShapeDtypeStruct((n_kv * piece_rows, 4 * width + LANES), BF16),
            jax.ShapeDtypeStruct((pad, 2 * width), F32),
        ),
        in_specs=[smem(), smem()] + [vmem()] * 9,
        out_specs=(vmem(), vmem()),
        scratch_shapes=[
            pltpu.VMEM((rows, 2 * width), BF16),
            pltpu.VMEM((rows, 2 * width), BF16),
        ],
        compiler_params=params(40),
        name="attend",
    )(
        dec_len, mix_lambda, normed, w_key, w_value, q_all, q_dec,
        ctx_keys, ctx_values, dec_keys, dec_values,
    )
    got = lax.all_to_all(send.reshape(n_kv, piece_rows, 4 * width + LANES), "kv", 0, 0)
    cols = w_out.shape[1] // n_tp
    extra = up(dec_rows * (cols // LANES), piece_rows) // piece_rows * LANES
    partial = pl.pallas_call(
        functools.partial(project_kernel, dec_rows=dec_rows, parts=n_tp),
        out_shape=jax.ShapeDtypeStruct((n_tp, piece_rows, cols + extra), BF16),
        in_specs=[smem()] + [vmem()] * 4,
        out_specs=vmem(),
        scratch_shapes=[pltpu.VMEM((rows, 2 * width), BF16)],
        compiler_params=params(12),
        name="project",
    )(mix_lambda, got, dec_att, head_gain.reshape(1, 2 * DH), w_out)
    me = lax.axis_index("tp")
    shares = [lax.dynamic_index_in_dim(partial, me, 0, keepdims=False)]
    for s in range(1, n_tp):
        mine = lax.dynamic_index_in_dim(partial, me ^ s, 0, keepdims=False)
        shares.append(lax.ppermute(mine, "tp", [(j, j ^ s) for j in range(n_tp)]))
    return pl.pallas_call(
        functools.partial(sum_kernel, dec_rows=dec_rows),
        out_shape=(
            jax.ShapeDtypeStruct((piece_rows, cols), BF16),
            jax.ShapeDtypeStruct((dec_rows, cols), BF16),
        ),
        in_specs=[vmem()] * n_tp,
        out_specs=(vmem(), vmem()),
        compiler_params=params(4),
        name="final_sum",
    )(*shares)


def solution(mesh):
    in_specs = (
        P("kv", None),
        P("kv", None),
        P(),
        P(None, None, "tp"),
        P(None, None, "tp"),
        P(None, "tp"),
        P("tp", None),
        P(),
        P("tp"),
        P(None, "kv", "tp"),
        P("kv", "tp"),
        P(None, "kv", None, "tp"),
        P("kv", None, "tp"),
        P("kv"),
    )
    out_specs = (P("kv", "tp"), P("kv", "tp"))
    run = functools.partial(body, n_kv=mesh.shape["kv"], n_tp=mesh.shape["tp"])
    return jax.shard_map(run, mesh=mesh, in_specs=in_specs, out_specs=out_specs, check_vma=False)
```
